32 devices in a mesh: kv: 8 (over z, y), tp: 4 (over x, core).
Axes of the slice: x: 2, y: 2, z: 4, core: 2. Of those that a mesh axis runs over, the one named last changes fastest.
Arguments:
- inputs: bfloat16 [256, 4096], P(None, 'kv'), may hold values from -150 to 150
- norm_gain: bfloat16 [4096], P('kv'), may hold values from 0.099609375 to 1.8984375
- w_query: bfloat16 [4096, 2048], P('kv', 'tp'), may hold values from -0.09375 to 0.09375
- w_forget: bfloat16 [4096, 2048], P('kv', 'tp'), may hold values from -0.09375 to 0.09375
- w_value: bfloat16 [4096, 2048], P('kv', 'tp'), may hold values from -0.09375 to 0.09375
- lower_bound: float32 [2048], P('tp'), may hold values from 0.05 to 0.9
- head_gain: float32 [2048], P('tp'), may hold values from 0.1 to 1.9
- w_out: bfloat16 [2048, 4096], P('tp', 'kv'), may hold values from -0.125 to 0.125
- prior_state: float32 [64, 16, 128, 128], P('kv', 'tp'), may hold values from -3 to 3
- prev_forget: float32 [64, 4, 2048], P('kv', None, 'tp'), may hold values from 0.3 to 0.97
- prev_values: bfloat16 [64, 4, 2048], P('kv', None, 'tp'), may hold values from -6 to 6
- accepted: int32 [64], P('kv'), may hold values from 0 to 4
Outputs:
- mixed_out: bfloat16 [256, 4096], P(None, ('kv', 'tp'))
- base_state: float32 [64, 16, 128, 128], P('kv', 'tp')
The draws below stay inside these ranges and needn't reach their ends.
All inputs are finite; a program needn't handle non-finite values.
Results may differ from the reference program's by a relative error of at most 0.01.
Values may be sent and summed in bfloat16 or wider, within the bound.
A program may use at most 64 MiB of HBM per device.

```python
import jax
import jax.numpy as jnp
from jax import lax

D = 4096
HEADS = 16
HEAD_SIZE = 128
PROPOSALS = 4
HEAD_WIDTH = 2048
SEQS = 64
TOKENS = 256
N_TP = 4


def draw_inputs(key, part):
    split_keys = jax.random.split(key, 4)
    column = jnp.arange(D, dtype=jnp.float32)[None, :] / D
    row_scale = 10.0 ** jax.random.uniform(split_keys[0], (TOKENS, 1), jnp.float32) / 3.0
    entries = jnp.clip(jax.random.normal(split_keys[1], (TOKENS, D), jnp.float32), -4.0, 4.0)
    column_scale = 10.0 ** (1.6 * column + 0.2 * jax.random.uniform(split_keys[3], (1, D), jnp.float32) - 0.9)
    return (entries * row_scale * column_scale).astype(jnp.bfloat16)


def set_ends(drawn, stream_key, smallest, largest):
    spot = [jax.random.randint(jax.random.fold_in(stream_key, axis), (), 0, length) for axis, length in enumerate(drawn.shape)]
    widest = drawn.shape.index(max(drawn.shape))
    beside = spot[:widest] + [(spot[widest] + 1) % drawn.shape[widest]] + spot[widest + 1:]
    return drawn.at[tuple(spot)].set(smallest).at[tuple(beside)].set(largest)


def shard_levels(rng, extent, pieces, low, high):
    factor_of = 1.0
    for dim, shards_of in pieces:
        draws = jax.random.uniform(jax.random.fold_in(jax.random.fold_in(rng, 6), dim), (shards_of,), jnp.float32, low / len(pieces), high / len(pieces))
        factor_of = factor_of * jnp.repeat(jnp.exp(draws), extent[dim] // shards_of).reshape((-1,) + (1,) * (len(extent) - 1 - dim))
    return factor_of


def normal_values(rng, extent, scale, reach, cuts=(), kind=jnp.bfloat16):
    result = scale * jax.random.normal(rng, extent, jnp.float32)
    if cuts:
        result = result * shard_levels(rng, extent, cuts, -0.22, 0.18)
    return jnp.clip(result, -reach, reach).astype(kind)


def setup_inputs(seed: int = 0) -> dict:
    seeds = jax.random.split(jax.random.key(seed), 13)
    return {
        "inputs": draw_inputs(jax.random.fold_in(seeds[12], 71), 0),
        "norm_gain": jnp.clip(1.0 + 0.18 * jax.random.normal(seeds[1], (D,), jnp.float32), 0.099609375, 1.8984375).astype(jnp.bfloat16),
        "w_query": normal_values(seeds[2], (D, HEAD_WIDTH), D ** -0.5, 0.09375, ((0, 8), (1, 4))),
        "w_forget": normal_values(seeds[3], (D, HEAD_WIDTH), D ** -0.5, 0.09375, ((0, 8), (1, 4))),
        "w_value": normal_values(seeds[4], (D, HEAD_WIDTH), D ** -0.5, 0.09375, ((0, 8), (1, 4))),
        "lower_bound": jnp.clip(0.05 + 0.84999998 * jax.random.uniform(seeds[5], (HEAD_WIDTH,), jnp.float32) ** shard_levels(seeds[5], (HEAD_WIDTH,), ((0, 4),), -0.2, 0.2), 0.05, 0.9),
        "head_gain": jnp.clip(1.0 + 0.18 * jax.random.normal(seeds[6], (HEAD_WIDTH,), jnp.float32), 0.1, 1.9),
        "w_out": normal_values(seeds[7], (HEAD_WIDTH, D), HEAD_WIDTH ** -0.5, 0.125, ((0, 4), (1, 8))),
        "prior_state": normal_values(seeds[8], (SEQS, HEADS, HEAD_SIZE, HEAD_SIZE), 0.5, 3.0, ((0, 8), (1, 4)), jnp.float32),
        "prev_forget": jnp.clip(0.3 + 0.67 * jax.random.uniform(seeds[9], (SEQS, PROPOSALS, HEAD_WIDTH), jnp.float32) ** shard_levels(seeds[9], (SEQS, PROPOSALS, HEAD_WIDTH), ((0, 8), (2, 4)), -0.2, 0.2), 0.3, 0.97),
        "prev_values": normal_values(seeds[10], (SEQS, PROPOSALS, HEAD_WIDTH), 1.0, 6.0, ((0, 8), (2, 4))),
        "accepted": set_ends(jax.random.randint(seeds[11], (SEQS,), 0, PROPOSALS + 1), jax.random.fold_in(seeds[11], 1), 0, PROPOSALS).astype(jnp.int32),
    }


EPSILON = 1e-06

def recurrence(query_pre, forget_pre, value_pre, lower_bound, head_gain, prior_state, prev_forget, prev_values, accepted):
    sequences = prior_state.shape[0]
    heads = prior_state.shape[1]
    head_size = prior_state.shape[2]
    proposals = prev_forget.shape[1]
    layout = (sequences, proposals, heads, head_size)
    floor_gate = lower_bound.reshape(heads, head_size)
    forget_gate = floor_gate + (1.0 - floor_gate) * jax.nn.sigmoid(forget_pre.reshape(layout))
    keys_new = 1.0 - forget_gate
    queries = jax.nn.silu(query_pre.reshape(layout))
    values = value_pre.reshape(layout)
    old_gate = prev_forget.reshape(layout)
    old_values = prev_values.astype(jnp.float32).reshape(layout)
    carried = prior_state
    for position in range(proposals):
        folded = old_gate[:, position, :, :, None] * carried + (1.0 - old_gate[:, position])[..., None] * old_values[:, position, :, None, :]
        taken_up = (position < accepted)[:, None, None, None]
        carried = jnp.where(taken_up, folded, carried)
    base_state = carried
    results = []
    for position in range(proposals):
        carried = forget_gate[:, position, :, :, None] * carried + keys_new[:, position, :, :, None] * values[:, position, :, None, :]
        results.append(jnp.einsum('shk,shkv->shv', queries[:, position], carried, precision=lax.Precision.HIGHEST))
    stacked = jnp.stack(results, axis=1)
    inverse_rms = lax.rsqrt(lax.optimization_barrier(jnp.mean(stacked * stacked, axis=-1, keepdims=True)) + EPSILON)
    normed = stacked * inverse_rms * head_gain.reshape(heads, head_size)
    return (normed.astype(jnp.bfloat16).reshape(sequences * proposals, heads * head_size), base_state)

def project(scaled, weight, rscale):
    return jnp.dot(scaled, weight, preferred_element_type=jnp.float32) * rscale[:, None]

def reference(inputs, norm_gain, w_query, w_forget, w_value, lower_bound, head_gain, w_out, prior_state, prev_forget, prev_values, accepted):
    widened = inputs.astype(jnp.float32)
    squares = lax.optimization_barrier(jnp.sum(widened * widened, axis=1))
    rscale = lax.rsqrt(squares / D + EPSILON)
    scaled = (widened * norm_gain.astype(jnp.float32)).astype(jnp.bfloat16)
    query_pre = project(scaled, w_query, rscale)
    forget_pre = project(scaled, w_forget, rscale)
    value_pre = project(scaled, w_value, rscale)
    normed, base_state = recurrence(query_pre, forget_pre, value_pre, lower_bound, head_gain, prior_state, prev_forget, prev_values, accepted)
    span_width = HEAD_WIDTH // N_TP
    mixed_out = jnp.zeros((TOKENS, D), jnp.float32)
    for member in range(N_TP):
        partial_value = jnp.dot(normed[:, member * span_width:(member + 1) * span_width], w_out[member * span_width:(member + 1) * span_width], preferred_element_type=jnp.float32)
        rounded = lax.optimization_barrier(partial_value.astype(jnp.bfloat16))
        mixed_out = mixed_out + rounded.astype(jnp.float32)
    return (mixed_out.astype(jnp.bfloat16), base_state)
```

```python
import functools

import jax
import jax.numpy as jnp
from jax import lax
from jax.experimental import pallas as pl
from jax.experimental.pallas import tpu as pltpu
from jax.sharding import PartitionSpec as P

EPSILON = 1e-06
MESH = pl.DeviceIdType.MESH
INNER = 2


def kernel(
    nkv,
    ntp,
    x_hbm,
    gain_hbm,
    wq_hbm,
    wf_hbm,
    wv_hbm,
    low_hbm,
    hgain_hbm,
    wout_hbm,
    state_hbm,
    gate_hbm,
    oldv_hbm,
    out_ref,
    base_hbm,
    x,
    gain,
    w,
    low,
    hgain,
    wout,
    state,
    stateb,
    gate,
    oldv,
    xs,
    sq_out,
    sq_in,
    a_out,
    a_in,
    keep,
    b_out,
    b_in,
    ag,
    t_out,
    t_in,
    load_sem,
    base_sem,
    sq_send,
    sq_recv,
    a_send,
    a_recv,
    b_send,
    b_recv,
    gz_send,
    gz_recv,
    gy_send,
    gy_recv,
    t_send,
    t_recv,
):
    nz = nkv // INNER
    heads, depth, width3 = w.shape
    size = width3 // 3
    rows = x.shape[2]
    seqs = state.shape[0]
    props = rows // seqs
    features = depth * nkv
    f32 = jnp.float32
    bf16 = jnp.bfloat16

    kv = lax.axis_index("kv")
    tp = lax.axis_index("tp")
    z = kv // INNER
    y = kv % INNER
    other = 1 - y

    def kv_at(d):
        return lax.rem(kv + d, nkv)

    def tp_at(d):
        return lax.rem(tp + d, ntp)

    def z_at(d):
        return lax.rem(z + d, nz)

    barrier = pltpu.get_barrier_semaphore()
    for d in range(1, nkv):
        pl.semaphore_signal(barrier, inc=1, device_id={"kv": kv_at(d)}, device_id_type=MESH)
    for d in range(1, ntp):
        pl.semaphore_signal(barrier, inc=1, device_id={"tp": tp_at(d)}, device_id_type=MESH)

    loads = {}

    def load(name, src, dst):
        copy = pltpu.make_async_copy(src, dst, load_sem.at[len(loads)])
        copy.start()
        loads[name] = copy

    load("x", x_hbm, x)
    load("gain", gain_hbm, gain)
    for h in range(heads):
        for n, src in enumerate((wq_hbm, wf_hbm, wv_hbm)):
            load(
                ("w", h, n),
                src.at[:, pl.ds(h * size, size)],
                w.at[h, :, pl.ds(n * size, size)],
            )
    load("gate", gate_hbm, gate)
    load("oldv", oldv_hbm, oldv)
    for h in range(heads):
        load(("state", h), state_hbm.at[:, h], state.at[:, h])
    load("low", low_hbm, low)
    load("hgain", hgain_hbm, hgain)
    load("wout", wout_hbm, wout)

    loads["x"].wait()
    loads["gain"].wait()
    eye = lax.broadcasted_iota(jnp.int32, (rows, size), 0) == lax.broadcasted_iota(
        jnp.int32, (rows, size), 1
    )
    gain_row = gain[...].astype(f32)
    for zz in range(nz):
        for yy in range(INNER):
            block = x[zz, yy].astype(f32)
            xs[zz, yy] = (block * gain_row).astype(bf16)
            column = jnp.sum(block * block, axis=1, keepdims=True)
            row = jnp.sum(jnp.where(eye, column, 0.0), axis=0, keepdims=True)
            sq_out[zz * INNER + yy] = jnp.broadcast_to(row, (8, size))

    xs_other = xs[:, other].reshape(nz * rows, depth)
    xs_mine = xs[:, y].reshape(nz * rows, depth)
    a_copies = []
    sq_copies = []
    for h in range(heads):
        for n in range(3):
            loads[("w", h, n)].wait()
        part = jnp.dot(xs_other, w[h], preferred_element_type=f32)
        a_out[h] = part.astype(bf16).reshape(nz, rows, width3)
        if h == 0:
            pl.semaphore_wait(barrier, nkv - 1 + ntp - 1)
            for d in range(1, nkv):
                copy = pltpu.make_async_remote_copy(
                    src_ref=sq_out.at[kv_at(d)],
                    dst_ref=sq_in.at[d - 1],
                    send_sem=sq_send.at[d - 1],
                    recv_sem=sq_recv.at[d - 1],
                    device_id={"kv": kv_at(d)},
                    device_id_type=MESH,
                )
                copy.start()
                sq_copies.append(copy)
        copy = pltpu.make_async_remote_copy(
            src_ref=a_out.at[h],
            dst_ref=a_in.at[h],
            send_sem=a_send.at[h],
            recv_sem=a_recv.at[h],
            device_id={"kv": z * INNER + other},
            device_id_type=MESH,
        )
        copy.start()
        a_copies.append(copy)
    for h in range(heads):
        part = jnp.dot(xs_mine, w[h], preferred_element_type=f32)
        keep[h] = part.reshape(nz, rows, width3)

    loads["gate"].wait()
    loads["oldv"].wait()
    gates = jnp.concatenate(
        [gate[:, h * size : (h + 1) * size] for h in range(heads)], axis=0
    )
    gates_t = gates.T
    base_copies = []
    b_copies = []
    for h in range(heads):
        loads[("state", h)].wait()
        for s in range(seqs):
            carried = state[s, h]
            for j in range(props):
                at = h * rows + s * props + j
                g = gates_t[:, at : at + 1]
                v = oldv[s * props + j : s * props + j + 1, h * size : (h + 1) * size]
                carried = g * carried + (1.0 - g) * v
            state[s, h] = carried
            stateb[s, h] = carried.astype(bf16)
        copy = pltpu.make_async_copy(state.at[:, h], base_hbm.at[:, h], base_sem.at[h])
        copy.start()
        base_copies.append(copy)

        a_copies[h].wait_recv()
        row_copies = []
        for d in range(1, nz):
            to = z_at(d)
            b_out[h, d - 1] = (keep[h, to] + a_in[h, to].astype(f32)).astype(bf16)
            copy = pltpu.make_async_remote_copy(
                src_ref=b_out.at[h, d - 1],
                dst_ref=b_in.at[h, d - 1],
                send_sem=b_send.at[h, d - 1],
                recv_sem=b_recv.at[h, d - 1],
                device_id={"kv": to * INNER + y},
                device_id_type=MESH,
            )
            copy.start()
            row_copies.append(copy)
        b_copies.append(row_copies)

    total = sq_out[kv]
    for d in range(1, nkv):
        sq_copies[d - 1].wait_recv()
        total = total + sq_in[d - 1]
    column = jnp.sum(jnp.where(eye, total[0:1], 0.0), axis=1, keepdims=True)
    rscale = lax.rsqrt(column / features + EPSILON)

    loads["low"].wait()
    loads["hgain"].wait()
    place = lax.broadcasted_iota(jnp.int32, (rows, size), 0)
    position = place % props
    half = lax.broadcasted_iota(jnp.int32, (8, size), 0) // props
    for h in range(heads):
        mine = keep[h, z] + a_in[h, z].astype(f32)
        for d in range(1, nz):
            b_copies[h][d - 1].wait_recv()
            mine = mine + b_in[h, d - 1].astype(f32)
        mine = mine * rscale
        query = mine[:, :size]
        query = query / (1.0 + jnp.exp(-query))
        floor = low[:, h * size : (h + 1) * size]
        forget = floor + (1.0 - floor) * jax.nn.sigmoid(mine[:, size : 2 * size])
        key = 1.0 - forget
        value = mine[:, 2 * size :]
        decay = query
        head_out = jnp.sum(query * key, axis=1, keepdims=True) * value
        for d in range(1, props):
            earlier = forget if d == 1 else pltpu.roll(forget, d - 1, 0)
            decay = decay * jnp.where(position >= d - 1, earlier, 1.0)
            weight = jnp.where(position >= d, decay * pltpu.roll(key, d, 0), 0.0)
            head_out = head_out + jnp.sum(weight, axis=1, keepdims=True) * pltpu.roll(
                value, d, 0
            )
        decay = decay * jnp.where(position >= props - 1, pltpu.roll(forget, props - 1, 0), 1.0)
        decay = decay.astype(bf16)
        per = 8 // props
        pieces = []
        for r in range(rows // 8):
            left = decay[r * 8 : (r + 1) * 8]
            piece = jnp.zeros((8, size), f32)
            for k in range(per):
                product = jnp.dot(left, stateb[r * per + k, h], preferred_element_type=f32)
                piece = jnp.where(half == k, product, piece)
            pieces.append(piece)
        head_out = head_out + jnp.concatenate(pieces, axis=0)
        mean = jnp.mean(head_out * head_out, axis=1, keepdims=True)
        normed = head_out * lax.rsqrt(mean + EPSILON) * hgain[:, h * size : (h + 1) * size]
        ag[z, y, :, h * size : (h + 1) * size] = normed.astype(bf16)

    def to_inner(slot, zz):
        copy = pltpu.make_async_remote_copy(
            src_ref=ag.at[zz, y],
            dst_ref=ag.at[zz, y],
            send_sem=gy_send.at[slot],
            recv_sem=gy_recv.at[slot],
            device_id={"kv": z * INNER + other},
            device_id_type=MESH,
        )
        copy.start()
        return copy

    gz_copies = []
    for d in range(1, nz):
        copy = pltpu.make_async_remote_copy(
            src_ref=ag.at[z, y],
            dst_ref=ag.at[z, y],
            send_sem=gz_send.at[d - 1],
            recv_sem=gz_recv.at[d - 1],
            device_id={"kv": z_at(d) * INNER + y},
            device_id_type=MESH,
        )
        copy.start()
        gz_copies.append(copy)
    gy_copies = [to_inner(0, z)]
    for d in range(1, nz):
        gz_copies[d - 1].wait_recv()
        gy_copies.append(to_inner(d, z_at(nz - d)))

    loads["wout"].wait()
    t_copies = []
    cols = out_ref.shape[3]
    for g in range(2):
        side = y if g == 0 else other
        if g == 1:
            for copy in gy_copies:
                copy.wait_recv()
        left = ag[:, side].reshape(nz * rows, heads * size)
        part = jnp.dot(left, wout[...], preferred_element_type=f32).astype(bf16)
        for t in range(ntp):
            t_out[g, t] = part[:, t * cols : (t + 1) * cols].reshape(nz, rows, cols)
        for d in range(1, ntp):
            copy = pltpu.make_async_remote_copy(
                src_ref=t_out.at[g, tp_at(d)],
                dst_ref=t_in.at[g, d - 1],
                send_sem=t_send.at[g, d - 1],
                recv_sem=t_recv.at[g, d - 1],
                device_id={"tp": tp_at(d)},
                device_id_type=MESH,
            )
            copy.start()
            t_copies.append(copy)
    for g in range(2):
        side = y if g == 0 else other
        acc = t_out[g, tp].astype(f32)
        for d in range(1, ntp):
            t_copies[g * (ntp - 1) + d - 1].wait_recv()
            acc = acc + t_in[g, d - 1].astype(f32)
        out_ref[:, side] = acc.astype(bf16)

    for copy in base_copies:
        copy.wait()
    for copy in sq_copies + a_copies + sum(b_copies, []) + gz_copies + gy_copies + t_copies:
        copy.wait_send()


def body(
    nkv,
    ntp,
    inputs,
    norm_gain,
    w_query,
    w_forget,
    w_value,
    lower_bound,
    head_gain,
    w_out,
    prior_state,
    prev_forget,
    prev_values,
    accepted,
):
    tokens, depth = inputs.shape
    seqs, heads, size, _ = prior_state.shape
    props = prev_forget.shape[1]
    rows = seqs * props
    width = heads * size
    nz = nkv // INNER
    cols = w_out.shape[1] // ntp
    taken = jnp.arange(props)[None, :, None] < accepted[:, None, None]
    gate = jnp.where(taken, prev_forget, 1.0).reshape(rows, width)
    oldv = prev_values.astype(jnp.float32).reshape(rows, width)
    f32, bf16 = jnp.float32, jnp.bfloat16
    dma = pltpu.SemaphoreType.DMA
    anywhere = pl.BlockSpec(memory_space=pl.ANY)
    mixed, base = pl.pallas_call(
        functools.partial(kernel, nkv, ntp),
        out_shape=(
            jax.ShapeDtypeStruct((nz, INNER, rows, cols), bf16),
            jax.ShapeDtypeStruct(prior_state.shape, f32),
        ),
        in_specs=[anywhere] * 11,
        out_specs=(pl.BlockSpec(memory_space=pltpu.VMEM), anywhere),
        scratch_shapes=[
            pltpu.VMEM((nz, INNER, rows, depth), bf16),
            pltpu.VMEM((1, depth), bf16),
            pltpu.VMEM((heads, depth, 3 * size), bf16),
            pltpu.VMEM((1, width), f32),
            pltpu.VMEM((1, width), f32),
            pltpu.VMEM(w_out.shape, bf16),
            pltpu.VMEM(prior_state.shape, f32),
            pltpu.VMEM(prior_state.shape, bf16),
            pltpu.VMEM((rows, width), f32),
            pltpu.VMEM((rows, width), f32),
            pltpu.VMEM((nz, INNER, rows, depth), bf16),
            pltpu.VMEM((nkv, 8, size), f32),
            pltpu.VMEM((nkv - 1, 8, size), f32),
            pltpu.VMEM((heads, nz, rows, 3 * size), bf16),
            pltpu.VMEM((heads, nz, rows, 3 * size), bf16),
            pltpu.VMEM((heads, nz, rows, 3 * size), f32),
            pltpu.VMEM((heads, nz - 1, rows, 3 * size), bf16),
            pltpu.VMEM((heads, nz - 1, rows, 3 * size), bf16),
            pltpu.VMEM((nz, INNER, rows, width), bf16),
            pltpu.VMEM((2, ntp, nz, rows, cols), bf16),
            pltpu.VMEM((2, ntp - 1, nz, rows, cols), bf16),
            dma((8 + 4 * heads,)),
            dma((heads,)),
            dma((nkv - 1,)),
            dma((nkv - 1,)),
            dma((heads,)),
            dma((heads,)),
            dma((heads, nz - 1)),
            dma((heads, nz - 1)),
            dma((nz - 1,)),
            dma((nz - 1,)),
            dma((nz,)),
            dma((nz,)),
            dma((2, ntp - 1)),
            dma((2, ntp - 1)),
        ],
        compiler_params=pltpu.CompilerParams(
            collective_id=0, has_side_effects=True, vmem_limit_bytes=60 * 1024 * 1024
        ),
    )(
        inputs.reshape(nz, INNER, rows, depth),
        norm_gain.reshape(1, depth),
        w_query,
        w_forget,
        w_value,
        lower_bound.reshape(1, width),
        head_gain.reshape(1, width),
        w_out,
        prior_state,
        gate,
        oldv,
    )
    return mixed.reshape(tokens, cols), base


def solution(mesh):
    in_specs = (
        P(None, "kv"),
        P("kv"),
        P("kv", "tp"),
        P("kv", "tp"),
        P("kv", "tp"),
        P("tp"),
        P("tp"),
        P("tp", "kv"),
        P("kv", "tp", None, None),
        P("kv", None, "tp"),
        P("kv", None, "tp"),
        P("kv"),
    )
    out_specs = (P(None, ("kv", "tp")), P("kv", "tp", None, None))
    return jax.shard_map(
        functools.partial(body, mesh.shape["kv"], mesh.shape["tp"]),
        mesh=mesh,
        in_specs=in_specs,
        out_specs=out_specs,
        check_vma=False,
    )
```

```python
import functools

import jax
import jax.numpy as jnp
from jax import lax
from jax.experimental import pallas as pl
from jax.experimental.pallas import tpu as pltpu
from jax.sharding import PartitionSpec as P

EPSILON = 1e-06
MESH = pl.DeviceIdType.MESH
INNER = 2


def kernel(
    nkv,
    ntp,
    x_hbm,
    gain_hbm,
    wq_hbm,
    wf_hbm,
    wv_hbm,
    low_hbm,
    hgain_hbm,
    wout_hbm,
    state_hbm,
    gate_hbm,
    oldv_hbm,
    accepted,
    out_ref,
    base_hbm,
    x,
    gain,
    w,
    low,
    hgain,
    wout,
    state,
    stateb,
    gate,
    gates,
    oldv,
    xs,
    sq_out,
    sq_in,
    a_out,
    a_in,
    keep,
    b_out,
    b_in,
    ag,
    t_out,
    t_in,
    load_sem,
    base_sem,
    sq_send,
    sq_recv,
    a_send,
    a_recv,
    b_send,
    b_recv,
    g_send,
    g_recv,
    t_send,
    t_recv,
):
    nz = nkv // INNER
    heads, depth, width3 = w.shape
    size = width3 // 3
    rows = x.shape[2]
    seqs = state.shape[0]
    props = rows // seqs
    features = depth * nkv
    f32 = jnp.float32
    bf16 = jnp.bfloat16

    kv = lax.axis_index("kv")
    tp = lax.axis_index("tp")
    z = kv // INNER
    y = kv % INNER
    other = 1 - y

    def kv_at(d):
        return lax.rem(kv + d, nkv)

    def tp_at(d):
        return lax.rem(tp + d, ntp)

    def z_at(d):
        return lax.rem(z + d, nz)

    barrier = pltpu.get_barrier_semaphore()
    for d in range(1, nkv):
        pl.semaphore_signal(barrier, inc=1, device_id={"kv": kv_at(d)}, device_id_type=MESH)
    for d in range(1, ntp):
        pl.semaphore_signal(barrier, inc=1, device_id={"tp": tp_at(d)}, device_id_type=MESH)

    loads = {}

    def load(name, src, dst):
        copy = pltpu.make_async_copy(src, dst, load_sem.at[len(loads)])
        copy.start()
        loads[name] = copy

    load("x", x_hbm, x)
    load("gain", gain_hbm, gain)
    for h in range(heads):
        for n, src in enumerate((wq_hbm, wf_hbm, wv_hbm)):
            load(
                ("w", h, n),
                src.at[:, pl.ds(h * size, size)],
                w.at[h, :, pl.ds(n * size, size)],
            )
    load("gate", gate_hbm, gate)
    load("oldv", oldv_hbm, oldv)
    for h in range(heads):
        load(("state", h), state_hbm.at[:, h], state.at[:, h])
    load("low", low_hbm, low)
    load("hgain", hgain_hbm, hgain)
    load("wout", wout_hbm, wout)

    loads["x"].wait()
    loads["gain"].wait()
    eye = lax.broadcasted_iota(jnp.int32, (rows, size), 0) == lax.broadcasted_iota(
        jnp.int32, (rows, size), 1
    )
    gain_row = gain[...].astype(f32).reshape(1, depth)
    for zz in range(nz):
        for yy in range(INNER):
            block = x[zz, yy].astype(f32)
            xs[zz, yy] = (block * gain_row).astype(bf16)
            column = jnp.sum(block * block, axis=1, keepdims=True)
            row = jnp.sum(jnp.where(eye, column, 0.0), axis=0, keepdims=True)
            sq_out[zz * INNER + yy] = jnp.broadcast_to(row, (8, size))

    xs_other = xs[:, other].reshape(nz * rows, depth)
    xs_mine = xs[:, y].reshape(nz * rows, depth)
    a_copies = []
    sq_copies = []
    for h in range(heads):
        for n in range(3):
            loads[("w", h, n)].wait()
        part = jnp.dot(xs_other, w[h], preferred_element_type=f32)
        a_out[h] = part.astype(bf16).reshape(nz, rows, width3)
        if h == 0:
            pl.semaphore_wait(barrier, nkv - 1 + ntp - 1)
            for d in range(1, nkv):
                copy = pltpu.make_async_remote_copy(
                    src_ref=sq_out.at[kv_at(d)],
                    dst_ref=sq_in.at[d - 1],
                    send_sem=sq_send.at[d - 1],
                    recv_sem=sq_recv.at[d - 1],
                    device_id={"kv": kv_at(d)},
                    device_id_type=MESH,
                )
                copy.start()
                sq_copies.append(copy)
        copy = pltpu.make_async_remote_copy(
            src_ref=a_out.at[h],
            dst_ref=a_in.at[h],
            send_sem=a_send.at[h],
            recv_sem=a_recv.at[h],
            device_id={"kv": z * INNER + other},
            device_id_type=MESH,
        )
        copy.start()
        a_copies.append(copy)
    for h in range(heads):
        part = jnp.dot(xs_mine, w[h], preferred_element_type=f32)
        keep[h] = part.reshape(nz, rows, width3)

    loads["gate"].wait()
    loads["oldv"].wait()
    order = lax.broadcasted_iota(jnp.int32, (props, heads * size), 0)
    for s in range(seqs):
        kept = jnp.where(order < accepted[s], gate[s], 1.0)
        for h in range(heads):
            gates[pl.ds(h * rows + s * props, props), :] = kept[:, h * size : (h + 1) * size]
    gates_t = gates[...].T
    base_copies = []
    b_copies = []
    for h in range(heads):
        loads[("state", h)].wait()
        for s in range(seqs):
            carried = state[s, h]
            values = oldv[s, :, h * size : (h + 1) * size].astype(f32)
            for j in range(props):
                at = h * rows + s * props + j
                g = gates_t[:, at : at + 1]
                carried = g * carried + (1.0 - g) * values[j : j + 1]
            state[s, h] = carried
            stateb[s, h] = carried.astype(bf16)
        copy = pltpu.make_async_copy(state.at[:, h], base_hbm.at[:, h], base_sem.at[h])
        copy.start()
        base_copies.append(copy)

        a_copies[h].wait_recv()
        row_copies = []
        for d in range(1, nz):
            to = z_at(d)
            b_out[h, d - 1] = (keep[h, to] + a_in[h, to].astype(f32)).astype(bf16)
            copy = pltpu.make_async_remote_copy(
                src_ref=b_out.at[h, d - 1],
                dst_ref=b_in.at[h, d - 1],
                send_sem=b_send.at[h, d - 1],
                recv_sem=b_recv.at[h, d - 1],
                device_id={"kv": to * INNER + y},
                device_id_type=MESH,
            )
            copy.start()
            row_copies.append(copy)
        b_copies.append(row_copies)

    total = sq_out[kv]
    for d in range(1, nkv):
        sq_copies[d - 1].wait_recv()
        total = total + sq_in[d - 1]
    column = jnp.sum(jnp.where(eye, total[0:1], 0.0), axis=1, keepdims=True)
    rscale = lax.rsqrt(column / features + EPSILON)

    loads["low"].wait()
    loads["hgain"].wait()
    place = lax.broadcasted_iota(jnp.int32, (rows, size), 0)
    position = place % props
    half = lax.broadcasted_iota(jnp.int32, (8, size), 0) // props
    g_copies = []

    def share(h, slot, zz, to):
        copy = pltpu.make_async_remote_copy(
            src_ref=ag.at[h, zz, y],
            dst_ref=ag.at[h, zz, y],
            send_sem=g_send.at[h, slot],
            recv_sem=g_recv.at[h, slot],
            device_id={"kv": to},
            device_id_type=MESH,
        )
        copy.start()
        return copy

    def pass_on(h):
        for d in range(1, nz):
            g_copies[h][d].wait_recv()
            g_copies[h].append(share(h, nz + d - 1, z_at(nz - d), z * INNER + other))

    for h in range(heads):
        mine = keep[h, z] + a_in[h, z].astype(f32)
        for d in range(1, nz):
            b_copies[h][d - 1].wait_recv()
            mine = mine + b_in[h, d - 1].astype(f32)
        mine = mine * rscale
        query = mine[:, :size]
        query = query / (1.0 + jnp.exp(-query))
        floor = low[:, h * size : (h + 1) * size]
        forget = floor + (1.0 - floor) * jax.nn.sigmoid(mine[:, size : 2 * size])
        key = 1.0 - forget
        value = mine[:, 2 * size :]
        decay = query
        head_out = jnp.sum(query * key, axis=1, keepdims=True) * value
        for d in range(1, props):
            earlier = forget if d == 1 else pltpu.roll(forget, d - 1, 0)
            decay = decay * jnp.where(position >= d - 1, earlier, 1.0)
            weight = jnp.where(position >= d, decay * pltpu.roll(key, d, 0), 0.0)
            head_out = head_out + jnp.sum(weight, axis=1, keepdims=True) * pltpu.roll(
                value, d, 0
            )
        decay = decay * jnp.where(position >= props - 1, pltpu.roll(forget, props - 1, 0), 1.0)
        decay = decay.astype(bf16)
        per = 8 // props
        pieces = []
        for r in range(rows // 8):
            left = decay[r * 8 : (r + 1) * 8]
            piece = jnp.zeros((8, size), f32)
            for k in range(per):
                product = jnp.dot(left, stateb[r * per + k, h], preferred_element_type=f32)
                piece = jnp.where(half == k, product, piece)
            pieces.append(piece)
        head_out = head_out + jnp.concatenate(pieces, axis=0)
        mean = jnp.mean(head_out * head_out, axis=1, keepdims=True)
        normed = head_out * lax.rsqrt(mean + EPSILON) * hgain[:, h * size : (h + 1) * size]
        ag[h, z, y] = normed.astype(bf16)
        copies = [share(h, 0, z, z * INNER + other)]
        for d in range(1, nz):
            copies.append(share(h, d, z, z_at(d) * INNER + y))
        g_copies.append(copies)
        if h:
            pass_on(h - 1)
    pass_on(heads - 1)

    loads["wout"].wait()
    t_copies = []
    cols = out_ref.shape[3]
    for g in range(2):
        side = y if g == 0 else other
        part = jnp.zeros((nz * rows, ntp * cols), f32)
        for h in range(heads):
            if g == 1:
                g_copies[h][0].wait_recv()
                for copy in g_copies[h][nz:]:
                    copy.wait_recv()
            left = ag[h, :, side].reshape(nz * rows, size)
            part = part + jnp.dot(
                left, wout[h * size : (h + 1) * size], preferred_element_type=f32
            )
        part = part.astype(bf16)
        for t in range(ntp):
            t_out[g, t] = part[:, t * cols : (t + 1) * cols].reshape(nz, rows, cols)
        for d in range(1, ntp):
            copy = pltpu.make_async_remote_copy(
                src_ref=t_out.at[g, tp_at(d)],
                dst_ref=t_in.at[g, d - 1],
                send_sem=t_send.at[g, d - 1],
                recv_sem=t_recv.at[g, d - 1],
                device_id={"tp": tp_at(d)},
                device_id_type=MESH,
            )
            copy.start()
            t_copies.append(copy)
    for g in range(2):
        side = y if g == 0 else other
        acc = t_out[g, tp].astype(f32)
        for d in range(1, ntp):
            t_copies[g * (ntp - 1) + d - 1].wait_recv()
            acc = acc + t_in[g, d - 1].astype(f32)
        out_ref[:, side] = acc.astype(bf16)

    for copy in base_copies:
        copy.wait()
    for copy in sq_copies + a_copies + sum(b_copies, []) + sum(g_copies, []) + t_copies:
        copy.wait_send()


def body(
    nkv,
    ntp,
    inputs,
    norm_gain,
    w_query,
    w_forget,
    w_value,
    lower_bound,
    head_gain,
    w_out,
    prior_state,
    prev_forget,
    prev_values,
    accepted,
):
    tokens, depth = inputs.shape
    seqs, heads, size, _ = prior_state.shape
    props = prev_forget.shape[1]
    rows = seqs * props
    width = heads * size
    nz = nkv // INNER
    cols = w_out.shape[1] // ntp
    f32, bf16 = jnp.float32, jnp.bfloat16
    dma = pltpu.SemaphoreType.DMA
    anywhere = pl.BlockSpec(memory_space=pl.ANY)
    mixed, base = pl.pallas_call(
        functools.partial(kernel, nkv, ntp),
        out_shape=(
            jax.ShapeDtypeStruct((nz, INNER, rows, cols), bf16),
            jax.ShapeDtypeStruct(prior_state.shape, f32),
        ),
        in_specs=[anywhere] * 11 + [pl.BlockSpec(memory_space=pltpu.SMEM)],
        out_specs=(pl.BlockSpec(memory_space=pltpu.VMEM), anywhere),
        scratch_shapes=[
            pltpu.VMEM((nz, INNER, rows, depth), bf16),
            pltpu.VMEM((depth,), bf16),
            pltpu.VMEM((heads, depth, 3 * size), bf16),
            pltpu.VMEM((1, width), f32),
            pltpu.VMEM((1, width), f32),
            pltpu.VMEM(w_out.shape, bf16),
            pltpu.VMEM(prior_state.shape, f32),
            pltpu.VMEM(prior_state.shape, bf16),
            pltpu.VMEM(prev_forget.shape, f32),
            pltpu.VMEM((heads * rows, size), f32),
            pltpu.VMEM(prev_values.shape, bf16),
            pltpu.VMEM((nz, INNER, rows, depth), bf16),
            pltpu.VMEM((nkv, 8, size), f32),
            pltpu.VMEM((nkv - 1, 8, size), f32),
            pltpu.VMEM((heads, nz, rows, 3 * size), bf16),
            pltpu.VMEM((heads, nz, rows, 3 * size), bf16),
            pltpu.VMEM((heads, nz, rows, 3 * size), f32),
            pltpu.VMEM((heads, nz - 1, rows, 3 * size), bf16),
            pltpu.VMEM((heads, nz - 1, rows, 3 * size), bf16),
            pltpu.VMEM((heads, nz, INNER, rows, size), bf16),
            pltpu.VMEM((2, ntp, nz, rows, cols), bf16),
            pltpu.VMEM((2, ntp - 1, nz, rows, cols), bf16),
            dma((8 + 4 * heads,)),
            dma((heads,)),
            dma((nkv - 1,)),
            dma((nkv - 1,)),
            dma((heads,)),
            dma((heads,)),
            dma((heads, nz - 1)),
            dma((heads, nz - 1)),
            dma((heads, 2 * nz - 1)),
            dma((heads, 2 * nz - 1)),
            dma((2, ntp - 1)),
            dma((2, ntp - 1)),
        ],
        compiler_params=pltpu.CompilerParams(
            collective_id=0, has_side_effects=True, vmem_limit_bytes=60 * 1024 * 1024
        ),
    )(
        inputs.reshape(nz, INNER, rows, depth),
        norm_gain,
        w_query,
        w_forget,
        w_value,
        lower_bound.reshape(1, width),
        head_gain.reshape(1, width),
        w_out,
        prior_state,
        prev_forget,
        prev_values,
        accepted,
    )
    return mixed.reshape(tokens, cols), base


def solution(mesh):
    in_specs = (
        P(None, "kv"),
        P("kv"),
        P("kv", "tp"),
        P("kv", "tp"),
        P("kv", "tp"),
        P("tp"),
        P("tp"),
        P("tp", "kv"),
        P("kv", "tp", None, None),
        P("kv", None, "tp"),
        P("kv", None, "tp"),
        P("kv"),
    )
    out_specs = (P(None, ("kv", "tp")), P("kv", "tp", None, None))
    return jax.shard_map(
        functools.partial(body, mesh.shape["kv"], mesh.shape["tp"]),
        mesh=mesh,
        in_specs=in_specs,
        out_specs=out_specs,
        check_vma=False,
    )
```

```python
import functools
import math

import jax
import jax.numpy as jnp
from jax import lax
from jax.experimental import pallas as pl
from jax.experimental.pallas import tpu as pltpu
from jax.sharding import PartitionSpec as P

EPSILON = 1e-06
MESH = pl.DeviceIdType.MESH
INNER = 2


def kernel(
    nkv,
    ntp,
    x_hbm,
    gain_hbm,
    wq_hbm,
    wf_hbm,
    wv_hbm,
    low_hbm,
    hgain_hbm,
    wout_hbm,
    state_hbm,
    gate_hbm,
    oldv_hbm,
    accepted_hbm,
    out_ref,
    base,
    x,
    gain,
    w,
    low,
    hgain,
    wout,
    state,
    stateb,
    gate,
    gates,
    oldv,
    accepted,
    xs,
    sq_out,
    sq_in,
    a_out,
    a_in,
    keep,
    b_out,
    b_in,
    ag,
    t_out,
    t_in,
    load_sem,
    sq_send,
    sq_recv,
    a_send,
    a_recv,
    b_send,
    b_recv,
    g_send,
    g_recv,
    t_send,
    t_recv,
):
    nz = nkv // INNER
    heads, depth, width3 = w.shape
    size = width3 // 3
    rows = x.shape[2]
    seqs = state.shape[0]
    props = rows // seqs
    features = depth * nkv
    f32 = jnp.float32
    bf16 = jnp.bfloat16

    kv = lax.axis_index("kv")
    tp = lax.axis_index("tp")
    z = kv // INNER
    y = kv % INNER
    other = 1 - y

    def kv_at(d):
        return lax.rem(kv + d, nkv)

    def tp_at(d):
        return lax.rem(tp + d, ntp)

    def z_at(d):
        return lax.rem(z + d, nz)

    barrier = pltpu.get_barrier_semaphore()
    for d in range(1, nkv):
        pl.semaphore_signal(barrier, inc=1, device_id={"kv": kv_at(d)}, device_id_type=MESH)
    for d in range(1, ntp):
        pl.semaphore_signal(barrier, inc=1, device_id={"tp": tp_at(d)}, device_id_type=MESH)

    loads = {}

    def load(name, src, dst):
        copy = pltpu.make_async_copy(src, dst, load_sem.at[len(loads)])
        copy.start()
        loads[name] = copy

    load("x", x_hbm, x)
    load("gain", gain_hbm, gain)
    for h in range(heads):
        for n, src in enumerate((wq_hbm, wf_hbm, wv_hbm)):
            load(
                ("w", h, n),
                src.at[:, pl.ds(h * size, size)],
                w.at[h, :, pl.ds(n * size, size)],
            )
    load("gate", gate_hbm, gate)
    load("oldv", oldv_hbm, oldv)
    load("accepted", accepted_hbm, accepted)
    for h in range(heads):
        load(("state", h), state_hbm.at[:, h], state.at[:, h])
    load("low", low_hbm, low)
    load("hgain", hgain_hbm, hgain)
    load("wout", wout_hbm, wout)

    loads["x"].wait()
    loads["gain"].wait()
    eye = lax.broadcasted_iota(jnp.int32, (rows, size), 0) == lax.broadcasted_iota(
        jnp.int32, (rows, size), 1
    )
    gain_row = gain[...].astype(f32).reshape(1, depth)
    for zz in range(nz):
        for yy in range(INNER):
            block = x[zz, yy].astype(f32)
            xs[zz, yy] = (block * gain_row).astype(bf16)
            column = jnp.sum(block * block, axis=1, keepdims=True)
            row = jnp.sum(jnp.where(eye, column, 0.0), axis=0, keepdims=True)
            sq_out[zz * INNER + yy] = jnp.broadcast_to(row, (8, size))

    xs_other = xs[:, other].reshape(nz * rows, depth)
    xs_mine = xs[:, y].reshape(nz * rows, depth)
    a_copies = []
    sq_copies = []
    for h in range(heads):
        for n in range(3):
            loads[("w", h, n)].wait()
        part = jnp.dot(xs_other, w[h], preferred_element_type=f32)
        a_out[h] = part.astype(bf16).reshape(nz, rows, width3)
        if h == 0:
            pl.semaphore_wait(barrier, nkv - 1 + ntp - 1)
            for d in range(1, nkv):
                copy = pltpu.make_async_remote_copy(
                    src_ref=sq_out.at[kv_at(d)],
                    dst_ref=sq_in.at[d - 1],
                    send_sem=sq_send.at[d - 1],
                    recv_sem=sq_recv.at[d - 1],
                    device_id={"kv": kv_at(d)},
                    device_id_type=MESH,
                )
                copy.start()
                sq_copies.append(copy)
        copy = pltpu.make_async_remote_copy(
            src_ref=a_out.at[h],
            dst_ref=a_in.at[h],
            send_sem=a_send.at[h],
            recv_sem=a_recv.at[h],
            device_id={"kv": z * INNER + other},
            device_id_type=MESH,
        )
        copy.start()
        a_copies.append(copy)
    for h in range(heads):
        part = jnp.dot(xs_mine, w[h], preferred_element_type=f32)
        keep[h] = part.reshape(nz, rows, width3)

    loads["gate"].wait()
    loads["oldv"].wait()
    loads["accepted"].wait()
    order = lax.broadcasted_iota(jnp.int32, (props, heads * size), 0)
    for s in range(seqs):
        kept = jnp.where(order < accepted[s], gate[s], 1.0)
        for h in range(heads):
            gates[pl.ds(h * rows + s * props, props), :] = kept[:, h * size : (h + 1) * size]
    gates_t = gates[...].T
    b_copies = []
    for h in range(heads):
        loads[("state", h)].wait()
        for s in range(seqs):
            carried = state[s, h]
            values = oldv[s, :, h * size : (h + 1) * size].astype(f32)
            for j in range(props):
                at = h * rows + s * props + j
                g = gates_t[:, at : at + 1]
                carried = g * carried + (1.0 - g) * values[j : j + 1]
            base[s, h] = carried
            stateb[s, h] = carried.astype(bf16)

        a_copies[h].wait_recv()
        row_copies = []
        for d in range(1, nz):
            to = z_at(d)
            b_out[h, d - 1] = (keep[h, to] + a_in[h, to].astype(f32)).astype(bf16)
            copy = pltpu.make_async_remote_copy(
                src_ref=b_out.at[h, d - 1],
                dst_ref=b_in.at[h, d - 1],
                send_sem=b_send.at[h, d - 1],
                recv_sem=b_recv.at[h, d - 1],
                device_id={"kv": to * INNER + y},
                device_id_type=MESH,
            )
            copy.start()
            row_copies.append(copy)
        b_copies.append(row_copies)

    total = sq_out[kv]
    for d in range(1, nkv):
        sq_copies[d - 1].wait_recv()
        total = total + sq_in[d - 1]
    column = jnp.sum(jnp.where(eye, total[0:1], 0.0), axis=1, keepdims=True)
    rscale = lax.rsqrt(column / features + EPSILON)

    loads["low"].wait()
    loads["hgain"].wait()
    place = lax.broadcasted_iota(jnp.int32, (rows, size), 0)
    position = place % props
    half = lax.broadcasted_iota(jnp.int32, (8, size), 0) // props
    g_copies = []

    def share(h, slot, zz, to):
        copy = pltpu.make_async_remote_copy(
            src_ref=ag.at[h, zz, y],
            dst_ref=ag.at[h, zz, y],
            send_sem=g_send.at[h, slot],
            recv_sem=g_recv.at[h, slot],
            device_id={"kv": to},
            device_id_type=MESH,
        )
        copy.start()
        return copy

    def pass_on(h):
        for d in range(1, nz):
            g_copies[h][d].wait_recv()
            g_copies[h].append(share(h, nz + d - 1, z_at(nz - d), z * INNER + other))

    for h in range(heads):
        mine = keep[h, z] + a_in[h, z].astype(f32)
        for d in range(1, nz):
            b_copies[h][d - 1].wait_recv()
            mine = mine + b_in[h, d - 1].astype(f32)
        mine = mine * rscale
        query = mine[:, :size]
        query = query / (1.0 + jnp.exp(-query))
        floor = low[:, h * size : (h + 1) * size]
        forget = floor + (1.0 - floor) * jax.nn.sigmoid(mine[:, size : 2 * size])
        key = 1.0 - forget
        value = mine[:, 2 * size :]
        decay = query
        head_out = jnp.sum(query * key, axis=1, keepdims=True) * value
        for d in range(1, props):
            earlier = forget if d == 1 else pltpu.roll(forget, d - 1, 0)
            decay = decay * jnp.where(position >= d - 1, earlier, 1.0)
            weight = jnp.where(position >= d, decay * pltpu.roll(key, d, 0), 0.0)
            head_out = head_out + jnp.sum(weight, axis=1, keepdims=True) * pltpu.roll(
                value, d, 0
            )
        decay = decay * jnp.where(position >= props - 1, pltpu.roll(forget, props - 1, 0), 1.0)
        decay = decay.astype(bf16)
        per = 8 // props
        pieces = []
        for r in range(rows // 8):
            left = decay[r * 8 : (r + 1) * 8]
            piece = jnp.zeros((8, size), f32)
            for k in range(per):
                product = jnp.dot(left, stateb[r * per + k, h], preferred_element_type=f32)
                piece = jnp.where(half == k, product, piece)
            pieces.append(piece)
        head_out = head_out + jnp.concatenate(pieces, axis=0)
        mean = jnp.mean(head_out * head_out, axis=1, keepdims=True)
        normed = head_out * lax.rsqrt(mean + EPSILON) * hgain[:, h * size : (h + 1) * size]
        ag[h, z, y] = normed.astype(bf16)
        copies = [share(h, 0, z, z * INNER + other)]
        for d in range(1, nz):
            copies.append(share(h, d, z, z_at(d) * INNER + y))
        g_copies.append(copies)
        if h:
            pass_on(h - 1)
    pass_on(heads - 1)

    loads["wout"].wait()
    t_copies = []
    cols = out_ref.shape[3]
    for g in range(2):
        side = y if g == 0 else other
        part = jnp.zeros((nz * rows, ntp * cols), f32)
        for h in range(heads):
            if g == 1:
                g_copies[h][0].wait_recv()
                for copy in g_copies[h][nz:]:
                    copy.wait_recv()
            left = ag[h, :, side].reshape(nz * rows, size)
            part = part + jnp.dot(
                left, wout[h * size : (h + 1) * size], preferred_element_type=f32
            )
        part = part.astype(bf16)
        for t in range(ntp):
            t_out[g, t] = part[:, t * cols : (t + 1) * cols].reshape(nz, rows, cols)
        for d in range(1, ntp):
            copy = pltpu.make_async_remote_copy(
                src_ref=t_out.at[g, tp_at(d)],
                dst_ref=t_in.at[g, d - 1],
                send_sem=t_send.at[g, d - 1],
                recv_sem=t_recv.at[g, d - 1],
                device_id={"tp": tp_at(d)},
                device_id_type=MESH,
            )
            copy.start()
            t_copies.append(copy)
    for g in range(2):
        side = y if g == 0 else other
        acc = t_out[g, tp].astype(f32)
        for d in range(1, ntp):
            t_copies[g * (ntp - 1) + d - 1].wait_recv()
            acc = acc + t_in[g, d - 1].astype(f32)
        out_ref[:, side] = acc.astype(bf16)

    for copy in sq_copies + a_copies + sum(b_copies, []) + sum(g_copies, []) + t_copies:
        copy.wait_send()


def body(
    nkv,
    ntp,
    inputs,
    norm_gain,
    w_query,
    w_forget,
    w_value,
    lower_bound,
    head_gain,
    w_out,
    prior_state,
    prev_forget,
    prev_values,
    accepted,
):
    tokens, depth = inputs.shape
    seqs, heads, size, _ = prior_state.shape
    props = prev_forget.shape[1]
    rows = seqs * props
    width = heads * size
    nz = nkv // INNER
    cols = w_out.shape[1] // ntp
    f32, bf16 = jnp.float32, jnp.bfloat16
    dma = pltpu.SemaphoreType.DMA
    anywhere = pl.BlockSpec(memory_space=pl.ANY)
    scratch = [
        pltpu.VMEM((nz, INNER, rows, depth), bf16),
        pltpu.VMEM((depth,), bf16),
        pltpu.VMEM((heads, depth, 3 * size), bf16),
        pltpu.VMEM((1, width), f32),
        pltpu.VMEM((1, width), f32),
        pltpu.VMEM(w_out.shape, bf16),
        pltpu.VMEM(prior_state.shape, f32),
        pltpu.VMEM(prior_state.shape, bf16),
        pltpu.VMEM(prev_forget.shape, f32),
        pltpu.VMEM((heads * rows, size), f32),
        pltpu.VMEM(prev_values.shape, bf16),
        pltpu.SMEM(accepted.shape, jnp.int32),
        pltpu.VMEM((nz, INNER, rows, depth), bf16),
        pltpu.VMEM((nkv, 8, size), f32),
        pltpu.VMEM((nkv - 1, 8, size), f32),
        pltpu.VMEM((heads, nz, rows, 3 * size), bf16),
        pltpu.VMEM((heads, nz, rows, 3 * size), bf16),
        pltpu.VMEM((heads, nz, rows, 3 * size), f32),
        pltpu.VMEM((heads, nz - 1, rows, 3 * size), bf16),
        pltpu.VMEM((heads, nz - 1, rows, 3 * size), bf16),
        pltpu.VMEM((heads, nz, INNER, rows, size), bf16),
        pltpu.VMEM((2, ntp, nz, rows, cols), bf16),
        pltpu.VMEM((2, ntp - 1, nz, rows, cols), bf16),
        dma((8 + 4 * heads,)),
        dma((nkv - 1,)),
        dma((nkv - 1,)),
        dma((heads,)),
        dma((heads,)),
        dma((heads, nz - 1)),
        dma((heads, nz - 1)),
        dma((heads, 2 * nz - 1)),
        dma((heads, 2 * nz - 1)),
        dma((2, ntp - 1)),
        dma((2, ntp - 1)),
    ]
    results = 4 * math.prod(prior_state.shape) + 2 * tokens * cols
    limit = 61 * 1024 * 1024 - results
    mixed, base = pl.pallas_call(
        functools.partial(kernel, nkv, ntp),
        out_shape=(
            pltpu.VMEM((nz, INNER, rows, cols), bf16),
            pltpu.VMEM(prior_state.shape, f32),
        ),
        in_specs=[anywhere] * 12,
        out_specs=(pl.BlockSpec(memory_space=pltpu.VMEM),) * 2,
        scratch_shapes=scratch,
        compiler_params=pltpu.CompilerParams(
            collective_id=0, has_side_effects=True, vmem_limit_bytes=limit
        ),
    )(
        inputs.reshape(nz, INNER, rows, depth),
        norm_gain,
        w_query,
        w_forget,
        w_value,
        lower_bound.reshape(1, width),
        head_gain.reshape(1, width),
        w_out,
        prior_state,
        prev_forget,
        prev_values,
        accepted,
    )
    return mixed.reshape(tokens, cols), base


def solution(mesh):
    in_specs = (
        P(None, "kv"),
        P("kv"),
        P("kv", "tp"),
        P("kv", "tp"),
        P("kv", "tp"),
        P("tp"),
        P("tp"),
        P("tp", "kv"),
        P("kv", "tp", None, None),
        P("kv", None, "tp"),
        P("kv", None, "tp"),
        P("kv"),
    )
    out_specs = (P(None, ("kv", "tp")), P("kv", "tp", None, None))
    return jax.shard_map(
        functools.partial(body, mesh.shape["kv"], mesh.shape["tp"]),
        mesh=mesh,
        in_specs=in_specs,
        out_specs=out_specs,
        check_vma=False,
    )
```
